128 devices in a mesh: fs: 16 (over z, y), tp: 8 (over x, core).
Axes of the slice: x: 4, y: 4, z: 4, core: 2. Of those that a mesh axis runs over, the one named last changes fastest.
Arguments:
- saved_input: bfloat16 [32768, 2048], P('fs'), may hold values from -6 to 6
- query_cotangent: bfloat16 [32768, 2048], P('fs', 'tp'), may hold values from -0.032958984 to 0.032958984
- forget_cotangent: bfloat16 [32768, 2048], P('fs', 'tp'), may hold values from -0.032958984 to 0.032958984
- mixed_output: bfloat16 [32768, 2048], P('fs', 'tp'), may hold values from -6 to 6
- out_cotangent: bfloat16 [32768, 2048], P('fs'), may hold values from -0.032958984 to 0.032958984
- query_basis: bfloat16 [2048, 256], replicated, may hold values from -0.125 to 0.125
- forget_basis: bfloat16 [2048, 256], replicated, may hold values from -0.125 to 0.125
- out_basis: bfloat16 [2048, 256], replicated, may hold values from -0.125 to 0.125
- query_weight: float32 [2048, 2048], P('fs', 'tp'), may hold values from -0.125 to 0.125
- forget_weight: float32 [2048, 2048], P('fs', 'tp'), may hold values from -0.125 to 0.125
- out_weight: float32 [2048, 2048], P('fs', 'tp'), may hold values from -0.125 to 0.125
- query_first: float32 [256, 2048], P('fs', 'tp'), may hold values from -25 to 25
- forget_first: float32 [256, 2048], P('fs', 'tp'), may hold values from -25 to 25
- out_first: float32 [256, 2048], P('fs', 'tp'), may hold values from -25 to 25
- query_second: float32 [256, 2048], P('fs', 'tp'), may hold values from 0.2 to 2
- forget_second: float32 [256, 2048], P('fs', 'tp'), may hold values from 0.2 to 2
- out_second: float32 [256, 2048], P('fs', 'tp'), may hold values from 0.2 to 2
Outputs:
- query_update: float32 [2048, 2048], P('fs', 'tp')
- forget_update: float32 [2048, 2048], P('fs', 'tp')
- out_update: float32 [2048, 2048], P('fs', 'tp')
- query_first_new: float32 [256, 2048], P('fs', 'tp')
- forget_first_new: float32 [256, 2048], P('fs', 'tp')
- out_first_new: float32 [256, 2048], P('fs', 'tp')
- query_second_new: float32 [256, 2048], P('fs', 'tp')
- forget_second_new: float32 [256, 2048], P('fs', 'tp')
- out_second_new: float32 [256, 2048], P('fs', 'tp')
- query_copy: bfloat16 [2048, 2048], P(None, 'tp')
- forget_copy: bfloat16 [2048, 2048], P(None, 'tp')
- out_copy: bfloat16 [2048, 2048], P(None, 'tp')
The draws below stay inside these ranges and needn't reach their ends.
All inputs are finite; a program needn't handle non-finite values.
Results may differ from the reference program's by a relative error of at most 0.0065.
Values may be sent and summed in bfloat16 or wider, within the bound.
No kernel may reach another device: no remote copies, remote signals or barrier semaphores. Data moves between devices by JAX's collectives and lax.ppermute only.
A program may use at most 128 MiB of HBM per device.

```python
import math
import jax
import jax.numpy as jnp
from jax import lax

D = 2048
WIDTH = 2048
RANK = 256
TOKENS = 32768


def moment_draw(key):
    key_rows = jax.random.fold_in(key, 11)
    key_cols = jax.random.fold_in(key, 12)
    key_base = jax.random.fold_in(key, 13)
    ramp_rows = jnp.arange(RANK, dtype=jnp.float32) / RANK
    ramp_cols = jnp.arange(WIDTH, dtype=jnp.float32) / WIDTH
    row_scale = jnp.exp(jnp.log(3.0) * (ramp_rows + jax.random.uniform(key_rows, (RANK,), jnp.float32)))
    col_scale = jnp.exp(jnp.log(3.0) * (ramp_cols + jax.random.uniform(key_cols, (WIDTH,), jnp.float32)))
    base = jnp.clip(jax.random.normal(key_base, (RANK, WIDTH), jnp.float32), -4.0, 4.0)
    return 0.075 * base * row_scale[:, None] * col_scale[None, :]


def draw_query_first(key, part):
    return moment_draw(jax.random.fold_in(key, 101))


def draw_forget_first(key, part):
    return moment_draw(jax.random.fold_in(key, 202))


def draw_out_first(key, part):
    return moment_draw(jax.random.fold_in(key, 303))


def block_scale(key, dims, split, low, high):
    level, own = 1.0, jax.random.fold_in(key, 6)
    for position, blocks in split:
        draws = jnp.exp(jax.random.uniform(jax.random.fold_in(own, position), (blocks,), jnp.float32, low / len(split), high / len(split)))
        level = level * jnp.repeat(draws, dims[position] // blocks).reshape([-1 if axis == position else 1 for axis in range(len(dims))])
    return level


def scatter_about(key, extent, scale, most, cuts=(), held_as=jnp.bfloat16):
    entries = jax.random.normal(key, extent, jnp.float32) * scale
    if len(cuts) > 0:
        entries = block_scale(key, extent, cuts, -0.22, 0.18) * entries
    return jnp.clip(entries, min=-most, max=most).astype(held_as)


def setup_inputs(seed: int = 0) -> dict:
    arg_keys = jax.random.split(jax.random.key(seed), 18)
    saved_input = scatter_about(arg_keys[0], (TOKENS, D), 1.0, 6.0, ((0, 16),))
    query_cotangent = scatter_about(arg_keys[1], (TOKENS, WIDTH), (TOKENS ** -0.5), 0.032958984, ((0, 16), (1, 8)))
    forget_cotangent = scatter_about(arg_keys[2], (TOKENS, WIDTH), (TOKENS ** -0.5), 0.032958984, ((0, 16), (1, 8)))
    mixed_output = scatter_about(arg_keys[3], (TOKENS, WIDTH), 1.0, 6.0, ((0, 16), (1, 8)))
    out_cotangent = scatter_about(arg_keys[4], (TOKENS, D), (TOKENS ** -0.5), 0.032958984, ((0, 16),))
    query_basis = scatter_about(arg_keys[5], (D, RANK), D ** -0.5, 0.125)
    forget_basis = scatter_about(arg_keys[6], (D, RANK), D ** -0.5, 0.125)
    out_basis = scatter_about(arg_keys[7], (D, RANK), D ** -0.5, 0.125)
    query_weight = scatter_about(arg_keys[8], (D, WIDTH), D ** -0.5, 0.125, ((0, 16), (1, 8)), jnp.float32)
    forget_weight = scatter_about(arg_keys[9], (D, WIDTH), D ** -0.5, 0.125, ((0, 16), (1, 8)), jnp.float32)
    out_weight = scatter_about(arg_keys[10], (D, WIDTH), WIDTH ** -0.5, 0.125, ((0, 16), (1, 8)), jnp.float32)
    query_first = draw_query_first(jax.random.fold_in(arg_keys[17], 71), 0)
    forget_first = draw_forget_first(jax.random.fold_in(arg_keys[17], 71), 0)
    out_first = draw_out_first(jax.random.fold_in(arg_keys[17], 71), 0)
    query_second = jnp.clip(jnp.exp(math.log(2.0) - 2.3025851 * jax.random.uniform(arg_keys[14], (RANK, WIDTH), jnp.float32) ** block_scale(arg_keys[14], (RANK, WIDTH), ((0, 16), (1, 8)), -0.2, 0.2)), 0.2, 2.0)
    forget_second = jnp.clip(jnp.exp(math.log(2.0) - 2.3025851 * jax.random.uniform(arg_keys[15], (RANK, WIDTH), jnp.float32) ** block_scale(arg_keys[15], (RANK, WIDTH), ((0, 16), (1, 8)), -0.2, 0.2)), 0.2, 2.0)
    out_second = jnp.clip(jnp.exp(math.log(2.0) - 2.3025851 * jax.random.uniform(arg_keys[16], (RANK, WIDTH), jnp.float32) ** block_scale(arg_keys[16], (RANK, WIDTH), ((0, 16), (1, 8)), -0.2, 0.2)), 0.2, 2.0)
    return {"saved_input": saved_input, "query_cotangent": query_cotangent, "forget_cotangent": forget_cotangent, "mixed_output": mixed_output, "out_cotangent": out_cotangent, "query_basis": query_basis, "forget_basis": forget_basis, "out_basis": out_basis, "query_weight": query_weight, "forget_weight": forget_weight, "out_weight": out_weight, "query_first": query_first, "forget_first": forget_first, "out_first": out_first, "query_second": query_second, "forget_second": forget_second, "out_second": out_second}


def one_matrix(source, cotangent, basis, weight, first, second):
    gradient = jnp.dot(source.T, cotangent, preferred_element_type=jnp.float32)
    basis_wide = basis.astype(jnp.float32)
    projected = jnp.dot(basis_wide.T, gradient, precision=lax.Precision.HIGHEST)
    first_new = 0.8 * first + 0.2 * projected
    second_new = 0.95 * second + 0.05 * projected * projected
    direction = first_new / (jnp.sqrt(second_new) + 1e-08)
    scale = lax.rsqrt(jnp.sum(direction * direction) / (RANK * WIDTH) + 1e-06)
    update = jnp.dot(basis_wide, direction, precision=lax.Precision.HIGHEST) * scale
    copy = (weight - 0.05 * update).astype(jnp.bfloat16)
    return (update, first_new, second_new, copy)

def reference(saved_input, query_cotangent, forget_cotangent, mixed_output, out_cotangent, query_basis, forget_basis, out_basis, query_weight, forget_weight, out_weight, query_first, forget_first, out_first, query_second, forget_second, out_second):
    q_update, q_first, q_second, q_copy = one_matrix(saved_input, query_cotangent, query_basis, query_weight, query_first, query_second)
    f_update, f_first, f_second, f_copy = one_matrix(saved_input, forget_cotangent, forget_basis, forget_weight, forget_first, forget_second)
    o_update, o_first, o_second, o_copy = one_matrix(out_cotangent, mixed_output, out_basis, out_weight, out_first, out_second)
    return (q_update, f_update, o_update, q_first, f_first, o_first, q_second, f_second, o_second, q_copy, f_copy, o_copy)
```

```python
import jax
import jax.numpy as jnp
from jax import lax
from jax.experimental import pallas as pl
from jax.experimental.pallas import tpu as pltpu
from jax.sharding import Mesh
from jax.sharding import PartitionSpec as P

WIDTH = 2048
RANK = 256
FS = ("fs_0", "fs_1")
TP = ("tp_0", "tp_1")
MATS = 3
TOKEN_BLOCK = 512
ROW_BLOCK = 256
VMEM_BYTES = 60 * 1024 * 1024

F32 = jnp.float32
BF16 = jnp.bfloat16


def whole(shape):
    return pl.BlockSpec(shape, lambda *_: (0,) * len(shape))


def cost(flops, moved):
    return pl.CostEstimate(flops=flops, bytes_accessed=moved, transcendentals=0)


def project_kernel(saved, grad, qb, fb, ob, qc, fc, mixed, out, *sums):
    step = pl.program_id(0)
    for total, source, basis, cotangent in zip(
        sums, (saved, saved, grad), (qb, fb, ob), (qc, fc, mixed)
    ):
        reduced = jnp.dot(source[...], basis[...], preferred_element_type=F32).astype(BF16)
        part = lax.dot_general(
            reduced, cotangent[...], (((0,), (0,)), ((), ())), preferred_element_type=F32
        )

        @pl.when(step == 0)
        def _():
            total[...] = part

        @pl.when(step > 0)
        def _():
            total[...] += part

    @pl.when(step == pl.num_programs(0) - 1)
    def _():
        groups, rows = out.shape[0], out.shape[1] // MATS
        for m, total in enumerate(sums):
            out[:, m * rows : (m + 1) * rows, :] = (
                total[...].astype(BF16).reshape(groups, rows, total.shape[1])
            )


def project(saved, grad, bases, cotangents, groups):
    tokens, width = saved.shape
    cols = cotangents[0].shape[1]
    rows = RANK // groups
    return pl.pallas_call(
        project_kernel,
        grid=(tokens // TOKEN_BLOCK,),
        in_specs=[
            pl.BlockSpec((TOKEN_BLOCK, width), lambda i: (i, 0)),
            pl.BlockSpec((TOKEN_BLOCK, width), lambda i: (i, 0)),
            *(whole((width, RANK)) for _ in bases),
            *(pl.BlockSpec((TOKEN_BLOCK, cols), lambda i: (i, 0)) for _ in cotangents),
        ],
        out_specs=whole((groups, MATS * rows, cols)),
        out_shape=jax.ShapeDtypeStruct((groups, MATS * rows, cols), BF16),
        scratch_shapes=[pltpu.VMEM((RANK, cols), F32) for _ in range(MATS)],
        compiler_params=pltpu.CompilerParams(vmem_limit_bytes=VMEM_BYTES),
        cost_estimate=cost(MATS * 2 * tokens * RANK * (width + cols), 22 << 20),
        name="project",
    )(saved, grad, *bases, *cotangents)


def moment_kernel(arrived, *refs):
    firsts, seconds = refs[:MATS], refs[MATS : 2 * MATS]
    firsts_new, seconds_new = refs[2 * MATS : 3 * MATS], refs[3 * MATS : 4 * MATS]
    directions = refs[4 * MATS]
    groups = arrived.shape[0]
    rows = arrived.shape[1] // MATS
    for m in range(MATS):
        at = slice(m * rows, (m + 1) * rows)
        projected = arrived[0, at, :].astype(F32)
        for g in range(1, groups):
            projected = projected + arrived[g, at, :].astype(F32)
        first_new = 0.8 * firsts[m][...] + 0.2 * projected
        second_new = 0.95 * seconds[m][...] + 0.05 * projected * projected
        firsts_new[m][...] = first_new
        seconds_new[m][...] = second_new
        direction = (first_new / (jnp.sqrt(second_new) + 1e-08)).astype(BF16)
        for g in range(groups):
            directions[g, at, :] = direction


def moments(arrived, firsts, seconds):
    state = [jax.ShapeDtypeStruct(a.shape, F32) for a in (*firsts, *seconds)]
    results = pl.pallas_call(
        moment_kernel,
        out_shape=(*state, jax.ShapeDtypeStruct(arrived.shape, BF16)),
        cost_estimate=cost(1 << 22, 1 << 20),
        name="moments",
    )(arrived, *firsts, *seconds)
    return results[:MATS], results[MATS : 2 * MATS], results[2 * MATS]


def square_kernel(gathered, out):
    rows = gathered.shape[1] // MATS
    out[...] = jnp.zeros_like(out)
    for m in range(MATS):
        values = gathered[:, m * rows : (m + 1) * rows, :].astype(F32)
        total = jnp.sum(values * values)
        out[m : m + 1, :] = jnp.full((1, out.shape[1]), total, F32)


def squares(gathered):
    return pl.pallas_call(
        square_kernel,
        out_shape=jax.ShapeDtypeStruct((8, 128), F32),
        cost_estimate=cost(1 << 22, 1 << 19),
        name="squares",
    )(gathered)


def expand_kernel(me, totals, gathered, qb, fb, ob, weights, *outs):
    updates, copies = outs[:MATS], outs[MATS:]
    step = pl.program_id(0)
    rows, cols = updates[0].shape
    rank_rows = gathered.shape[1] // MATS
    for m, basis in enumerate((qb, fb, ob)):
        direction = gathered[:, m * rank_rows : (m + 1) * rank_rows, :].reshape(RANK, cols)
        total = totals[m : m + 1, :1]
        scale = lax.rsqrt(total * (1.0 / (RANK * WIDTH)) + 1e-06)

        @pl.when(step == 0)
        def _():
            mine = basis[pl.ds(pl.multiple_of(me[0] * rows, rows), rows), :]
            updates[m][...] = jnp.dot(mine, direction, preferred_element_type=F32) * scale

        at = pl.ds(pl.multiple_of(step * ROW_BLOCK, ROW_BLOCK), ROW_BLOCK)
        stepped = jnp.dot(basis[at, :], direction, preferred_element_type=F32)
        weight = weights[:, m * cols : (m + 1) * cols].astype(F32)
        copies[m][...] = (weight - 0.05 * (stepped * scale)).astype(BF16)


def expand(me, totals, gathered, bases, weights, rows):
    width = bases[0].shape[0]
    cols = gathered.shape[2]
    return pl.pallas_call(
        expand_kernel,
        grid_spec=pltpu.PrefetchScalarGridSpec(
            num_scalar_prefetch=1,
            grid=(width // ROW_BLOCK,),
            in_specs=[
                whole(totals.shape),
                whole(gathered.shape),
                *(whole((width, RANK)) for _ in bases),
                pl.BlockSpec((ROW_BLOCK, MATS * cols), lambda i, *_: (i, 0)),
            ],
            out_specs=[
                *(whole((rows, cols)) for _ in range(MATS)),
                *(pl.BlockSpec((ROW_BLOCK, cols), lambda i, *_: (i, 0)) for _ in range(MATS)),
            ],
        ),
        out_shape=[
            *(jax.ShapeDtypeStruct((rows, cols), F32) for _ in range(MATS)),
            *(jax.ShapeDtypeStruct((width, cols), BF16) for _ in range(MATS)),
        ],
        compiler_params=pltpu.CompilerParams(vmem_limit_bytes=VMEM_BYTES),
        cost_estimate=cost(MATS * 2 * width * RANK * cols, 9 << 20),
        name="expand",
    )(me, totals, gathered, *bases, weights)


def summed_over_tp(value):
    for axis, far in (("tp_1", 1), ("tp_0", 1), ("tp_0", 2)):
        size = lax.axis_size(axis)
        value = value + lax.ppermute(value, axis, [(i, i ^ far) for i in range(size)])
    return value


def local(
    saved_input,
    query_cotangent,
    forget_cotangent,
    mixed_output,
    out_cotangent,
    query_basis,
    forget_basis,
    out_basis,
    query_weight,
    forget_weight,
    out_weight,
    *state,
):
    rows = query_weight.shape[0]
    groups = lax.axis_size(FS)
    bases = (query_basis, forget_basis, out_basis)
    weights = jnp.concatenate(
        [w.astype(BF16) for w in (query_weight, forget_weight, out_weight)], axis=1
    )
    all_weights = lax.all_gather(weights, FS, axis=0, tiled=True)
    blocks = project(
        saved_input,
        out_cotangent,
        bases,
        (query_cotangent, forget_cotangent, mixed_output),
        groups,
    )
    arrived = lax.all_to_all(blocks, FS, 0, 0, tiled=True)
    firsts, seconds, directions = moments(arrived, state[:MATS], state[MATS:])
    gathered = lax.all_to_all(directions, FS, 0, 0, tiled=True)
    totals = summed_over_tp(squares(gathered))
    me = lax.axis_index(FS).astype(jnp.int32).reshape(1)
    outs = expand(me, totals, gathered, bases, all_weights, rows)
    return (*outs[:MATS], *firsts, *seconds, *outs[MATS:])


def solution(mesh):
    split = Mesh(mesh.devices.reshape(4, 4, 4, 2), ("fs_0", "fs_1", "tp_0", "tp_1"))
    in_specs = (
        P(FS, None),
        P(FS, TP),
        P(FS, TP),
        P(FS, TP),
        P(FS, None),
        P(),
        P(),
        P(),
        *(P(FS, TP) for _ in range(9)),
    )
    out_specs = (*(P(FS, TP) for _ in range(9)), *(P(None, TP) for _ in range(3)))
    return jax.shard_map(local, mesh=split, in_specs=in_specs, out_specs=out_specs, check_vma=False)
```

```python
import functools

import jax
import jax.numpy as jnp
from jax import lax
from jax.experimental import pallas as pl
from jax.experimental.pallas import tpu as pltpu
from jax.sharding import Mesh
from jax.sharding import PartitionSpec as P

WIDTH = 2048
RANK = 256
FS = ("fs_0", "fs_1")
TP = ("tp_0", "tp_1")
MATS = 3
IN_CUTS = (0, 512, 2048)
OUT_CUTS = (0, 512, 2048)
SIDE = 4
SMALL_GRANT = 24 * 1024 * 1024
REDUCE_GRANT = 56 * 1024 * 1024
MOMENT_GRANT = 60 * 1024 * 1024
LARGE_GRANT = 60 * 1024 * 1024

F32 = jnp.float32
BF16 = jnp.bfloat16

FAR = ((0, 0), (2, 0), (0, 2), (2, 2))
NEAR = ((0, 0), (1, 0), (0, 1), (3, 3))


def cost(flops, moved):
    return pl.CostEstimate(flops=flops, bytes_accessed=moved, transcendentals=0)


def params(grant=SMALL_GRANT):
    return pltpu.CompilerParams(vmem_limit_bytes=grant)


def round_kernel(*refs):
    out = refs[MATS]
    cols = refs[0].shape[1]
    for m in range(MATS):
        out[:, m * cols : (m + 1) * cols] = refs[m][...].astype(BF16)


def rounded(weights):
    rows, cols = weights[0].shape
    return pl.pallas_call(
        round_kernel,
        out_shape=jax.ShapeDtypeStruct((rows, MATS * cols), BF16),
        compiler_params=params(LARGE_GRANT),
        cost_estimate=cost(1 << 20, 1 << 19),
        name="rounded",
    )(*weights)


def reduce_kernel(count, cuts, core, source, *refs):
    bases, out = refs[:count], refs[count]
    rows_in, basis_in, sums, sems = refs[count + 1 :]
    half = out.shape[0]
    mine = pl.ds(pl.multiple_of(core[0] * half, half), half)
    copies = []
    for c, (low, high) in enumerate(zip(cuts, cuts[1:])):
        at = slice(low, high)
        pieces = [(source.at[mine, at], rows_in.at[:, at])]
        pieces += [(bases[m].at[at, :], basis_in.at[m, at, :]) for m in range(count)]
        copies.append(
            [pltpu.make_async_copy(a, b, sems.at[c, p]) for p, (a, b) in enumerate(pieces)]
        )
        for copy in copies[-1]:
            copy.start()
    for c, (low, high) in enumerate(zip(cuts, cuts[1:])):
        at = slice(low, high)
        for copy in copies[c]:
            copy.wait()
        for m in range(count):
            to = slice(m * RANK, (m + 1) * RANK)
            part = jnp.dot(rows_in[:, at], basis_in[m, at, :], preferred_element_type=F32)
            if c > 0:
                part = sums[:, to] + part
            if c < len(cuts) - 2:
                sums[:, to] = part
            else:
                out[:, to] = part.astype(BF16)


def reduce_half(core, source, bases, cuts):
    tokens, width = source.shape
    half, count = tokens // 2, len(bases)
    anywhere = pl.BlockSpec(memory_space=pl.ANY)
    return pl.pallas_call(
        functools.partial(reduce_kernel, count, cuts),
        in_specs=[
            pl.BlockSpec(memory_space=pltpu.SMEM),
            *(anywhere for _ in range(1 + count)),
        ],
        out_specs=pl.BlockSpec(memory_space=pltpu.VMEM),
        scratch_shapes=[
            pltpu.VMEM((half, width), BF16),
            pltpu.VMEM((count, width, RANK), BF16),
            pltpu.VMEM((half, count * RANK), F32),
            pltpu.SemaphoreType.DMA((len(cuts) - 1, 1 + count)),
        ],
        out_shape=jax.ShapeDtypeStruct((half, count * RANK), BF16),
        compiler_params=params(REDUCE_GRANT),
        cost_estimate=cost(2 * half * RANK * width * count, 6 << 20),
    )(core, source, *bases)


def contract_rows(left, right):
    return lax.dot_general(
        left, right, (((0,), (0,)), ((), ())), preferred_element_type=F32
    )


def contract_near_kernel(core, own, other, own_out, qc, fc, mixed, out):
    half = own.shape[0]
    mine = pl.ds(pl.multiple_of(core[0] * half, half), half)
    theirs = pl.ds(pl.multiple_of((1 - core[0]) * half, half), half)
    for m, cotangent in enumerate((qc, fc)):
        at = slice(m * RANK, (m + 1) * RANK)
        out[m] = contract_rows(own[:, at], cotangent[mine, :]) + contract_rows(
            other[:, at], cotangent[theirs, :]
        )
    out[2] = contract_rows(own_out[...], mixed[mine, :])


def contract_far_kernel(core, sums, other_out, mixed, out):
    half = other_out.shape[0]
    theirs = pl.ds(pl.multiple_of((1 - core[0]) * half, half), half)
    groups, rows = out.shape[0], out.shape[1] // MATS
    last = sums[2] + contract_rows(other_out[...], mixed[theirs, :])
    for m, total in enumerate((sums[0], sums[1], last)):
        out[:, m * rows : (m + 1) * rows, :] = total.astype(BF16).reshape(
            groups, rows, total.shape[1]
        )


def contract(core, own, other, own_out, other_out, cotangents, groups):
    cols = cotangents[0].shape[1]
    half = own.shape[0]
    smem = pl.BlockSpec(memory_space=pltpu.SMEM)
    vmem = pl.BlockSpec(memory_space=pltpu.VMEM)
    sums = pl.pallas_call(
        contract_near_kernel,
        in_specs=[smem, *(vmem for _ in range(6))],
        out_specs=vmem,
        out_shape=jax.ShapeDtypeStruct((MATS, RANK, cols), F32),
        compiler_params=params(),
        cost_estimate=cost(5 * 2 * half * RANK * cols, 6 << 20),
        name="contract_near",
    )(core, own, other, own_out, *cotangents)
    return pl.pallas_call(
        contract_far_kernel,
        in_specs=[smem, *(vmem for _ in range(3))],
        out_specs=vmem,
        out_shape=jax.ShapeDtypeStruct((groups, MATS * (RANK // groups), cols), BF16),
        compiler_params=params(),
        cost_estimate=cost(2 * half * RANK * cols, 1 << 20),
        name="contract_far",
    )(core, sums, other_out, cotangents[2])


def moment_kernel(arrived, *refs):
    state, state_new = refs[: 2 * MATS], refs[2 * MATS : 4 * MATS]
    directions, held, sems = refs[4 * MATS :]
    groups = arrived.shape[0]
    rows = arrived.shape[1] // MATS
    copies = [
        pltpu.make_async_copy(state[n], held.at[n], sems.at[n]) for n in range(2 * MATS)
    ]
    for copy in copies:
        copy.start()
    projected = arrived[0].astype(F32)
    for g in range(1, groups):
        projected = projected + arrived[g].astype(F32)
    for copy in copies:
        copy.wait()
    for m in range(MATS):
        at = slice(m * rows, (m + 1) * rows)
        value = projected[at]
        first_new = 0.8 * held[m] + 0.2 * value
        second_new = 0.95 * held[MATS + m] + 0.05 * value * value
        state_new[m][...] = first_new
        state_new[MATS + m][...] = second_new
        direction = (first_new / (jnp.sqrt(second_new) + 1e-08)).astype(BF16)
        for g in range(groups):
            directions[g, at, :] = direction


def moments(arrived, state):
    vmem = pl.BlockSpec(memory_space=pltpu.VMEM)
    anywhere = pl.BlockSpec(memory_space=pl.ANY)
    results = pl.pallas_call(
        moment_kernel,
        in_specs=[vmem, *(anywhere for _ in state)],
        out_specs=[vmem for _ in range(1 + len(state))],
        out_shape=[
            *(jax.ShapeDtypeStruct(a.shape, F32) for a in state),
            jax.ShapeDtypeStruct(arrived.shape, BF16),
        ],
        scratch_shapes=[
            pltpu.VMEM((len(state), *state[0].shape), F32),
            pltpu.SemaphoreType.DMA((len(state),)),
        ],
        compiler_params=params(MOMENT_GRANT),
        cost_estimate=cost(1 << 22, 1 << 20),
        name="moments",
    )(arrived, *state)
    return results[: len(state)], results[len(state)]


def square_kernel(gathered, out):
    rows = gathered.shape[1] // MATS
    out[...] = jnp.zeros_like(out)
    for m in range(MATS):
        values = gathered[:, m * rows : (m + 1) * rows, :].astype(F32)
        total = jnp.sum(values * values)
        out[m : m + 1, :] = jnp.full((1, out.shape[1]), total, F32)


def squares(gathered):
    return pl.pallas_call(
        square_kernel,
        out_shape=jax.ShapeDtypeStruct((8, 128), F32),
        compiler_params=params(),
        cost_estimate=cost(1 << 22, 1 << 19),
        name="squares",
    )(gathered)


def step_kernel(gathered, qb, fb, ob, out):
    rank_rows, cols = gathered.shape[1] // MATS, gathered.shape[2]
    for m, basis in enumerate((qb, fb, ob)):
        direction = gathered[:, m * rank_rows : (m + 1) * rank_rows, :].reshape(RANK, cols)

        def piece(i, carry):
            at = pl.ds(pl.multiple_of(i * 512, 512), 512)
            out[m, at, :] = jnp.dot(basis[at, :], direction, preferred_element_type=F32)
            return carry

        lax.fori_loop(0, basis.shape[0] // 512, piece, 0)


def steps(gathered, bases):
    width, cols = bases[0].shape[0], gathered.shape[2]
    return pl.pallas_call(
        step_kernel,
        out_shape=jax.ShapeDtypeStruct((MATS, width, cols), F32),
        compiler_params=params(),
        cost_estimate=cost(MATS * 2 * width * RANK * cols, 9 << 20),
        name="steps",
    )(gathered, *bases)


def apply_kernel(me, totals, stepped, *refs):
    weights = refs[: len(NEAR)]
    updates = refs[len(NEAR) : len(NEAR) + MATS]
    copies = refs[len(NEAR) + MATS :]
    rows, cols = updates[0].shape
    scales = [
        lax.rsqrt(totals[m : m + 1, :1] * (1.0 / (RANK * WIDTH)) + 1e-06) for m in range(MATS)
    ]
    mine = pl.ds(pl.multiple_of((me[0] * SIDE + me[1]) * rows, rows), rows)
    for m in range(MATS):
        updates[m][...] = stepped[m, mine, :] * scales[m]

    def block(j, carry):
        far = (2 * lax.rem(j, 2), 2 * lax.div(j, 2))
        for near, weight in zip(NEAR, weights):
            z = lax.rem(me[0] + 2 * SIDE - near[0] - far[0], SIDE)
            y = lax.rem(me[1] + 2 * SIDE - near[1] - far[1], SIDE)
            at = pl.ds(pl.multiple_of((z * SIDE + y) * rows, rows), rows)
            for m in range(MATS):
                old = weight[j, :, m * cols : (m + 1) * cols].astype(F32)
                new = old - 0.05 * (stepped[m, at, :] * scales[m])
                copies[m][at, :] = new.astype(BF16)
        return carry

    lax.fori_loop(0, len(FAR), block, 0)


def applied(me, totals, stepped, weights, rows):
    width, cols = stepped.shape[1:]
    smem = pl.BlockSpec(memory_space=pltpu.SMEM)
    vmem = pl.BlockSpec(memory_space=pltpu.VMEM)
    return pl.pallas_call(
        apply_kernel,
        in_specs=[smem, *(vmem for _ in range(2 + len(weights)))],
        out_specs=[vmem for _ in range(2 * MATS)],
        out_shape=[
            *(jax.ShapeDtypeStruct((rows, cols), F32) for _ in range(MATS)),
            *(jax.ShapeDtypeStruct((width, cols), BF16) for _ in range(MATS)),
        ],
        compiler_params=params(),
        cost_estimate=cost(1 << 24, 12 << 20),
        name="applied",
    )(me, totals, stepped, *weights)


def moved_by(value, offset):
    pairs = []
    for z in range(SIDE):
        for y in range(SIDE):
            target = ((z + offset[0]) % SIDE) * SIDE + (y + offset[1]) % SIDE
            pairs.append((z * SIDE + y, target))
    return lax.ppermute(value, FS, pairs)


def gathered_by(value, offsets):
    moved = []
    for offset in offsets[1:]:
        moved.append(moved_by(value, offset))
    return moved


def summed_over_tp(value):
    value = value + lax.ppermute(value, "tp_1", [(0, 1), (1, 0)])
    arrived = [
        lax.ppermute(value, "tp_0", [(i, (i + far) % SIDE) for i in range(SIDE)])
        for far in (1, 2, 3)
    ]
    return value + (arrived[0] + arrived[2]) + arrived[1]


def body(
    saved_input,
    query_cotangent,
    forget_cotangent,
    mixed_output,
    out_cotangent,
    query_basis,
    forget_basis,
    out_basis,
    query_weight,
    forget_weight,
    out_weight,
    *state,
):
    rows = query_weight.shape[0]
    groups = lax.axis_size(FS)
    bases = (query_basis, forget_basis, out_basis)
    cotangents = (query_cotangent, forget_cotangent, mixed_output)
    core = lax.axis_index("tp_1").astype(jnp.int32).reshape(1)
    me = jnp.stack([lax.axis_index("fs_0"), lax.axis_index("fs_1")]).astype(jnp.int32)
    swap = [(0, 1), (1, 0)]

    weights = rounded((query_weight, forget_weight, out_weight))
    four = jnp.stack([weights, *gathered_by(weights, FAR)])
    all_weights = (four, *gathered_by(four, NEAR))

    own = reduce_half(core, saved_input, bases[:2], IN_CUTS)
    other = lax.ppermute(own, "tp_1", swap)
    own_out = reduce_half(core, out_cotangent, bases[2:], OUT_CUTS)
    other_out = lax.ppermute(own_out, "tp_1", swap)
    blocks = contract(core, own, other, own_out, other_out, cotangents, groups)

    arrived = lax.all_to_all(blocks, FS, 0, 0, tiled=True)
    state_new, directions = moments(arrived, state)
    gathered = lax.all_to_all(directions, FS, 0, 0, tiled=True)
    totals = summed_over_tp(squares(gathered))
    stepped = steps(gathered, bases)
    outs = applied(me, totals, stepped, all_weights, rows)
    return (*outs[:MATS], *state_new, *outs[MATS:])


def solution(mesh):
    split = Mesh(mesh.devices.reshape(4, 4, 4, 2), ("fs_0", "fs_1", "tp_0", "tp_1"))
    in_specs = (
        P(FS, None),
        P(FS, TP),
        P(FS, TP),
        P(FS, TP),
        P(FS, None),
        P(),
        P(),
        P(),
        *(P(FS, TP) for _ in range(9)),
    )
    out_specs = (*(P(FS, TP) for _ in range(9)), *(P(None, TP) for _ in range(3)))
    return jax.shard_map(body, mesh=split, in_specs=in_specs, out_specs=out_specs, check_vma=False)
```

```python
import functools

import jax
import jax.numpy as jnp
from jax import lax
from jax.experimental import pallas as pl
from jax.experimental.pallas import tpu as pltpu
from jax.sharding import Mesh
from jax.sharding import PartitionSpec as P

WIDTH = 2048
RANK = 256
FS = ("fs_0", "fs_1")
TP = ("tp_0", "tp_1")
MATS = 3
IN_CUTS = (0, 512, 2048)
OUT_CUTS = (0, 512, 2048)
SIDE = 4
GRANT = 24 * 1024 * 1024

F32 = jnp.float32
BF16 = jnp.bfloat16

FAR = ((0, 0), (2, 0), (0, 2), (2, 2))
NEAR = ((0, 0), (1, 0), (0, 1), (3, 3))


SMEM = pl.BlockSpec(memory_space=pltpu.SMEM)
VMEM = pl.BlockSpec(memory_space=pltpu.VMEM)
HBM = pl.BlockSpec(memory_space=pltpu.HBM)


def cost(flops, moved):
    return pl.CostEstimate(flops=flops, bytes_accessed=moved, transcendentals=0)


def params():
    return pltpu.CompilerParams(vmem_limit_bytes=GRANT)


def in_hbm(*arrays):
    return [pltpu.with_memory_space_constraint(a, pltpu.HBM) for a in arrays]


def in_vmem(*arrays):
    return [pltpu.with_memory_space_constraint(a, pltpu.VMEM) for a in arrays]


def contract_rows(left, right):
    return lax.dot_general(
        left, right, (((0,), (0,)), ((), ())), preferred_element_type=F32
    )


def half_of(which, half):
    return pl.ds(pl.multiple_of(which * half, half), half)


def reduce_in_kernel(core, source, qb, fb, qw, fw, ow, *refs):
    state, (out, rounded, packed) = refs[: 2 * MATS], refs[2 * MATS : 2 * MATS + 3]
    rows_in, basis_in, weights_in, sums, sems, weight_sems, state_sems = refs[2 * MATS + 3 :]
    bases, weights = (qb, fb), (qw, fw, ow)
    mine = half_of(core[0], out.shape[0])
    copies = []
    for c, (low, high) in enumerate(zip(IN_CUTS, IN_CUTS[1:])):
        at = slice(low, high)
        pieces = [(source.at[mine, at], rows_in.at[:, at])]
        pieces += [(b.at[at, :], basis_in.at[m, at, :]) for m, b in enumerate(bases)]
        copies.append(
            [pltpu.make_async_copy(a, b, sems.at[c, p]) for p, (a, b) in enumerate(pieces)]
        )
    weight_copies = [
        pltpu.make_async_copy(w, weights_in.at[m], weight_sems.at[m])
        for m, w in enumerate(weights)
    ]
    state_copies = [
        pltpu.make_async_copy(a, packed.at[n], state_sems.at[n]) for n, a in enumerate(state)
    ]
    for copy in (*copies[0], *weight_copies, *copies[1], *state_copies):
        copy.start()
    for c, (low, high) in enumerate(zip(IN_CUTS, IN_CUTS[1:])):
        at = slice(low, high)
        for copy in copies[c]:
            copy.wait()
        for m in range(len(bases)):
            to = slice(m * RANK, (m + 1) * RANK)
            part = jnp.dot(rows_in[:, at], basis_in[m, at, :], preferred_element_type=F32)
            if c == 0:
                sums[:, to] = part
            else:
                out[:, to] = (sums[:, to] + part).astype(BF16)
        if c == 0:
            cols = weights_in.shape[2]
            for m, copy in enumerate(weight_copies):
                copy.wait()
                rounded[:, m * cols : (m + 1) * cols] = weights_in[m].astype(BF16)
    for copy in state_copies:
        copy.wait()


def reduce_in(core, source, bases, weights, state):
    tokens, width = source.shape
    half, count = tokens // 2, len(bases)
    rows, cols = weights[0].shape
    return pl.pallas_call(
        reduce_in_kernel,
        in_specs=[SMEM, *(HBM for _ in range(1 + count + MATS + len(state)))],
        out_specs=[VMEM, VMEM, VMEM],
        out_shape=[
            pltpu.VMEM((half, count * RANK), BF16),
            pltpu.VMEM((rows, MATS * cols), BF16),
            pltpu.VMEM((len(state), *state[0].shape), F32),
        ],
        scratch_shapes=[
            pltpu.VMEM((half, width), BF16),
            pltpu.VMEM((count, width, RANK), BF16),
            pltpu.VMEM((MATS, rows, cols), F32),
            pltpu.VMEM((half, count * RANK), F32),
            pltpu.SemaphoreType.DMA((len(IN_CUTS) - 1, 1 + count)),
            pltpu.SemaphoreType.DMA((MATS,)),
            pltpu.SemaphoreType.DMA((len(state),)),
        ],
        compiler_params=params(),
        cost_estimate=cost(2 * half * RANK * width * count, 6 << 20),
        name="reduce_in",
    )(core, *in_hbm(source, *bases, *weights, *state))


def reduce_out_kernel(core, own, qc, fc, mixed, source, basis, out, sums, *scratch):
    rows_in, basis_in, total, sems = scratch
    mine = half_of(core[0], out.shape[0])
    copies = []
    for c, (low, high) in enumerate(zip(OUT_CUTS, OUT_CUTS[1:])):
        at = slice(low, high)
        copies.append(
            [
                pltpu.make_async_copy(source.at[mine, at], rows_in.at[:, at], sems.at[c, 0]),
                pltpu.make_async_copy(basis.at[at, :], basis_in.at[at, :], sems.at[c, 1]),
            ]
        )
        for copy in copies[c]:
            copy.start()
    for m, cotangent in enumerate((qc, fc)):
        sums[m] = contract_rows(own[:, m * RANK : (m + 1) * RANK], cotangent[mine, :])
    for c, (low, high) in enumerate(zip(OUT_CUTS, OUT_CUTS[1:])):
        at = slice(low, high)
        for copy in copies[c]:
            copy.wait()
        part = jnp.dot(rows_in[:, at], basis_in[at, :], preferred_element_type=F32)
        if c == 0:
            total[...] = part
        else:
            out[...] = (total[...] + part).astype(BF16)
    sums[2] = contract_rows(out[...], mixed[mine, :])


def reduce_out(core, own, cotangents, source, basis):
    tokens, width = source.shape
    half, cols = tokens // 2, cotangents[0].shape[1]
    return pl.pallas_call(
        reduce_out_kernel,
        in_specs=[SMEM, *(VMEM for _ in range(1 + MATS)), HBM, HBM],
        out_specs=[VMEM, VMEM],
        out_shape=[pltpu.VMEM((half, RANK), BF16), pltpu.VMEM((MATS, RANK, cols), F32)],
        scratch_shapes=[
            pltpu.VMEM((half, width), BF16),
            pltpu.VMEM((width, RANK), BF16),
            pltpu.VMEM((half, RANK), F32),
            pltpu.SemaphoreType.DMA((len(OUT_CUTS) - 1, 2)),
        ],
        compiler_params=params(),
        cost_estimate=cost(2 * half * RANK * (width + 3 * cols), 6 << 20),
        name="reduce_out",
    )(core, *in_vmem(own, *cotangents), *in_hbm(source, basis))


def contract_kernel(picked, core, sums, other, *refs):
    cotangents = refs[: len(picked)]
    out, held, sems = refs[-3:]
    groups, rows = out.shape[0], out.shape[1] // MATS
    theirs = half_of(1 - core[0], other.shape[0])
    copies = []
    for k, (m, cotangent) in enumerate(zip(picked, cotangents)):
        total = sums[m] + contract_rows(
            other[:, k * RANK : (k + 1) * RANK], cotangent[theirs, :]
        )
        held[k] = total.astype(BF16).reshape(groups, rows, total.shape[1])
        copies.append(
            pltpu.make_async_copy(
                held.at[k], out.at[:, m * rows : (m + 1) * rows, :], sems.at[k]
            )
        )
        copies[k].start()
    for copy in copies:
        copy.wait()


def contract(picked, core, sums, other, cotangents, groups, into):
    cols = sums.shape[2]
    rows = RANK // groups
    count = len(picked)
    earlier = [] if into is None else in_hbm(into)
    return pl.pallas_call(
        functools.partial(contract_kernel, picked),
        in_specs=[SMEM, *(VMEM for _ in range(2 + count)), *(HBM for _ in earlier)],
        out_specs=HBM,
        out_shape=pltpu.HBM((groups, MATS * rows, cols), BF16),
        scratch_shapes=[
            pltpu.VMEM((count, groups, rows, cols), BF16),
            pltpu.SemaphoreType.DMA((count,)),
        ],
        input_output_aliases={3 + count: 0} if earlier else {},
        compiler_params=params(),
        cost_estimate=cost(2 * count * other.shape[0] * RANK * cols, count << 20),
    )(core, *in_vmem(sums, other, *(cotangents[m] for m in picked)), *earlier)


def moment_kernel(arrived, held, *refs):
    state_new = refs[: 2 * MATS]
    directions, direction, sems = refs[2 * MATS :]
    groups = arrived.shape[0]
    rows = arrived.shape[1] // MATS
    for m in range(MATS):
        at = slice(m * rows, (m + 1) * rows)
        value = arrived[0, at, :].astype(F32)
        for g in range(1, groups):
            value = value + arrived[g, at, :].astype(F32)
        first_new = 0.8 * held[m] + 0.2 * value
        second_new = 0.95 * held[MATS + m] + 0.05 * value * value
        state_new[m][...] = first_new
        state_new[MATS + m][...] = second_new
        direction[at, :] = (first_new / (jnp.sqrt(second_new) + 1e-08)).astype(BF16)
    sends = [
        pltpu.make_async_copy(direction, directions.at[g], sems.at[g]) for g in range(groups)
    ]
    for send in sends:
        send.start()
    for send in sends:
        send.wait()


def moments(arrived, packed):
    groups, rows, cols = arrived.shape
    count = packed.shape[0]
    results = pl.pallas_call(
        moment_kernel,
        in_specs=[VMEM, VMEM],
        out_specs=[*(VMEM for _ in range(count)), HBM],
        out_shape=[
            *(jax.ShapeDtypeStruct(packed.shape[1:], F32) for _ in range(count)),
            pltpu.HBM(arrived.shape, BF16),
        ],
        scratch_shapes=[
            pltpu.VMEM((rows, cols), BF16),
            pltpu.SemaphoreType.DMA((groups,)),
        ],
        compiler_params=params(),
        cost_estimate=cost(1 << 22, 1 << 20),
        name="moments",
    )(*in_vmem(arrived, packed))
    return results[:count], results[count]


def collect_kernel(*refs):
    for k, block in enumerate(refs[: len(FAR)]):
        refs[len(FAR)][k] = block[...]


def collected(blocks):
    return pl.pallas_call(
        collect_kernel,
        in_specs=[VMEM for _ in blocks],
        out_specs=VMEM,
        out_shape=pltpu.HBM((len(blocks), *blocks[0].shape), BF16),
        compiler_params=params(),
        cost_estimate=cost(1 << 20, 2 << 20),
        name="collected",
    )(*in_vmem(*blocks))


def square_kernel(gathered, out):
    rows = gathered.shape[1] // MATS
    out[...] = jnp.zeros_like(out)
    for m in range(MATS):
        values = gathered[:, m * rows : (m + 1) * rows, :].astype(F32)
        total = jnp.sum(values * values)
        out[m : m + 1, :] = jnp.full((1, out.shape[1]), total, F32)


def squares(gathered):
    return pl.pallas_call(
        square_kernel,
        out_shape=jax.ShapeDtypeStruct((8, 128), F32),
        compiler_params=params(),
        cost_estimate=cost(1 << 22, 1 << 19),
        name="squares",
    )(gathered)


def step_kernel(gathered, qb, fb, ob, out):
    rank_rows, cols = gathered.shape[1] // MATS, gathered.shape[2]
    for m, basis in enumerate((qb, fb, ob)):
        direction = gathered[:, m * rank_rows : (m + 1) * rank_rows, :].reshape(RANK, cols)

        def piece(i, carry):
            at = pl.ds(pl.multiple_of(i * 512, 512), 512)
            out[m, at, :] = jnp.dot(basis[at, :], direction, preferred_element_type=F32)
            return carry

        lax.fori_loop(0, basis.shape[0] // 512, piece, 0)


def steps(gathered, bases):
    width, cols = bases[0].shape[0], gathered.shape[2]
    return pl.pallas_call(
        step_kernel,
        out_shape=jax.ShapeDtypeStruct((MATS, width, cols), F32),
        compiler_params=params(),
        cost_estimate=cost(MATS * 2 * width * RANK * cols, 9 << 20),
        name="steps",
    )(gathered, *bases)


def apply_kernel(me, totals, stepped, *refs):
    weights = refs[: len(NEAR)]
    updates = refs[len(NEAR) : len(NEAR) + MATS]
    copies = refs[len(NEAR) + MATS : len(NEAR) + 2 * MATS]
    stepped_own, held, sems = refs[len(NEAR) + 2 * MATS :]
    rows, cols = stepped_own.shape[1:]
    mine = pl.ds(pl.multiple_of((me[0] * SIDE + me[1]) * rows, rows), rows)
    stores = []
    for m in range(MATS):
        total = totals[m : m + 1, :1]
        scale = lax.rsqrt(total * (1.0 / (RANK * WIDTH)) + 1e-06)
        factor = 0.05 * scale
        stepped_own[m] = stepped[m, mine, :] * scale

        def block(j, carry):
            far_z, far_y = 2 * lax.rem(j, 2), 2 * lax.div(j, 2)
            for near, weight in zip(NEAR, weights):
                z = lax.rem(me[0] + 2 * SIDE - near[0] - far_z, SIDE)
                y = lax.rem(me[1] + 2 * SIDE - near[1] - far_y, SIDE)
                at = pl.ds(pl.multiple_of((z * SIDE + y) * rows, rows), rows)
                old = weight[j, :, m * cols : (m + 1) * cols].astype(F32)
                held[m, at, :] = (old - factor * stepped[m, at, :]).astype(BF16)
            return carry

        lax.fori_loop(0, len(FAR), block, 0)
        stores.append(pltpu.make_async_copy(held.at[m], copies[m], sems.at[m]))
        stores.append(pltpu.make_async_copy(stepped_own.at[m], updates[m], sems.at[MATS + m]))
        stores[-2].start()
        stores[-1].start()
    for store in stores:
        store.wait()


def applied(me, totals, stepped, weights, rows):
    width, cols = stepped.shape[1:]
    return pl.pallas_call(
        apply_kernel,
        in_specs=[SMEM, *(VMEM for _ in range(2 + len(weights)))],
        out_specs=[HBM for _ in range(2 * MATS)],
        out_shape=[
            *(pltpu.HBM((rows, cols), F32) for _ in range(MATS)),
            *(pltpu.HBM((width, cols), BF16) for _ in range(MATS)),
        ],
        scratch_shapes=[
            pltpu.VMEM((MATS, rows, cols), F32),
            pltpu.VMEM((MATS, width, cols), BF16),
            pltpu.SemaphoreType.DMA((2 * MATS,)),
        ],
        compiler_params=params(),
        cost_estimate=cost(1 << 24, 12 << 20),
        name="applied",
    )(me, *in_vmem(totals, stepped, *weights))


def moved_by(value, offset):
    pairs = []
    for z in range(SIDE):
        for y in range(SIDE):
            target = ((z + offset[0]) % SIDE) * SIDE + (y + offset[1]) % SIDE
            pairs.append((z * SIDE + y, target))
    return lax.ppermute(value, FS, pairs)


def gathered_by(value, offsets):
    moved = []
    for offset in offsets[1:]:
        moved.append(moved_by(value, offset))
    return moved


def summed_over_tp(value):
    value = value + lax.ppermute(value, "tp_1", [(0, 1), (1, 0)])
    arrived = [
        lax.ppermute(value, "tp_0", [(i, (i + far) % SIDE) for i in range(SIDE)])
        for far in (1, 2, 3)
    ]
    return value + (arrived[0] + arrived[2]) + arrived[1]


def body(
    saved_input,
    query_cotangent,
    forget_cotangent,
    mixed_output,
    out_cotangent,
    query_basis,
    forget_basis,
    out_basis,
    query_weight,
    forget_weight,
    out_weight,
    *state,
):
    rows = query_weight.shape[0]
    groups = lax.axis_size(FS)
    bases = (query_basis, forget_basis, out_basis)
    cotangents = (query_cotangent, forget_cotangent, mixed_output)
    core = lax.axis_index("tp_1").astype(jnp.int32).reshape(1)
    me = jnp.stack([lax.axis_index("fs_0"), lax.axis_index("fs_1")]).astype(jnp.int32)

    own, weights, packed = reduce_in(
        core, saved_input, bases[:2], (query_weight, forget_weight, out_weight), state
    )
    other = lax.ppermute(own, "tp_1", [(0, 1), (1, 0)])
    own_out, sums = reduce_out(core, own, cotangents, out_cotangent, out_basis)
    other_out = lax.ppermute(own_out, "tp_1", [(0, 1), (1, 0)])
    blocks = contract((0, 1), core, sums, other, cotangents, groups, None)
    blocks = contract((2,), core, sums, other_out, cotangents, groups, blocks)
    four = collected((weights, *gathered_by(weights, FAR)))
    all_weights = (four, *gathered_by(four, NEAR))
    arrived = lax.all_to_all(blocks, FS, 0, 0, tiled=True)
    state_new, directions = moments(arrived, packed)
    gathered = lax.all_to_all(directions, FS, 0, 0, tiled=True)
    totals = summed_over_tp(squares(gathered))
    stepped = steps(gathered, bases)
    outs = applied(me, totals, stepped, all_weights, rows)
    return (*outs[:MATS], *state_new, *outs[MATS:])


def solution(mesh):
    split = Mesh(mesh.devices.reshape(4, 4, 4, 2), ("fs_0", "fs_1", "tp_0", "tp_1"))
    in_specs = (
        P(FS, None),
        P(FS, TP),
        P(FS, TP),
        P(FS, TP),
        P(FS, None),
        P(),
        P(),
        P(),
        *(P(FS, TP) for _ in range(9)),
    )
    out_specs = (*(P(FS, TP) for _ in range(9)), *(P(None, TP) for _ in range(3)))
    return jax.shard_map(body, mesh=split, in_specs=in_specs, out_specs=out_specs, check_vma=False)
```

```python
import jax
import jax.numpy as jnp
from jax import lax
from jax.experimental import pallas as pl
from jax.experimental.pallas import tpu as pltpu
from jax.sharding import Mesh
from jax.sharding import PartitionSpec as P

WIDTH = 2048
RANK = 256
FS = ("fs_0", "fs_1")
TP = ("tp_0", "tp_1")
MATS = 3
IN_CUTS = (0, 512, 2048)
SIDE = 4
GRANT = 24 * 1024 * 1024

F32 = jnp.float32
BF16 = jnp.bfloat16

FAR = ((0, 0), (2, 0), (0, 2), (2, 2))
NEAR = ((0, 0), (3, 0), (0, 3), (1, 1))


SMEM = pl.BlockSpec(memory_space=pltpu.SMEM)
VMEM = pl.BlockSpec(memory_space=pltpu.VMEM)
HBM = pl.BlockSpec(memory_space=pltpu.HBM)


def cost(flops, moved):
    return pl.CostEstimate(flops=flops, bytes_accessed=moved, transcendentals=0)


def params():
    return pltpu.CompilerParams(vmem_limit_bytes=GRANT)


def in_hbm(*arrays):
    return [pltpu.with_memory_space_constraint(a, pltpu.HBM) for a in arrays]


def in_vmem(*arrays):
    return [pltpu.with_memory_space_constraint(a, pltpu.VMEM) for a in arrays]


def contract_rows(left, right):
    return lax.dot_general(
        left, right, (((0,), (0,)), ((), ())), preferred_element_type=F32
    )


def half_of(which, half):
    return pl.ds(pl.multiple_of(which * half, half), half)


def reduce_in_kernel(core, source, qb, fb, qw, fw, ow, grad, ob, *refs):
    state, refs = refs[: 2 * MATS], refs[2 * MATS :]
    out, rounded, packed, grad_half, ob_held = refs[:5]
    rows_in, basis_in, weights_in, sums, sems, weight_sems, state_sems, next_sems = refs[5:]
    bases, weights = (qb, fb), (qw, fw, ow)
    mine = half_of(core[0], out.shape[0])
    copies = []
    for c, (low, high) in enumerate(zip(IN_CUTS, IN_CUTS[1:])):
        at = slice(low, high)
        pieces = [(source.at[mine, at], rows_in.at[:, at])]
        pieces += [(b.at[at, :], basis_in.at[m, at, :]) for m, b in enumerate(bases)]
        copies.append(
            [pltpu.make_async_copy(a, b, sems.at[c, p]) for p, (a, b) in enumerate(pieces)]
        )
    weight_copies = [
        pltpu.make_async_copy(w, weights_in.at[m], weight_sems.at[m])
        for m, w in enumerate(weights)
    ]
    state_copies = [
        pltpu.make_async_copy(a, packed.at[n], state_sems.at[n]) for n, a in enumerate(state)
    ]
    next_copies = [
        pltpu.make_async_copy(grad.at[mine, :], grad_half, next_sems.at[0]),
        pltpu.make_async_copy(ob, ob_held, next_sems.at[1]),
    ]
    for copy in (*copies[0], *weight_copies, *copies[1]):
        copy.start()
    for c, (low, high) in enumerate(zip(IN_CUTS, IN_CUTS[1:])):
        at = slice(low, high)
        for copy in copies[c]:
            copy.wait()
        if c > 0:
            for copy in (*next_copies, *state_copies):
                copy.start()
        for m in range(len(bases)):
            to = slice(m * RANK, (m + 1) * RANK)
            part = jnp.dot(rows_in[:, at], basis_in[m, at, :], preferred_element_type=F32)
            if c == 0:
                sums[:, to] = part
            else:
                out[:, to] = (sums[:, to] + part).astype(BF16)
        if c == 0:
            cols = weights_in.shape[2]
            for m, copy in enumerate(weight_copies):
                copy.wait()
                rounded[:, m * cols : (m + 1) * cols] = weights_in[m].astype(BF16)
    for copy in (*state_copies, *next_copies):
        copy.wait()


def reduce_in(core, source, bases, weights, grad, ob, state):
    tokens, width = source.shape
    half, count = tokens // 2, len(bases)
    rows, cols = weights[0].shape
    return pl.pallas_call(
        reduce_in_kernel,
        in_specs=[SMEM, *(HBM for _ in range(3 + count + MATS + len(state)))],
        out_specs=[VMEM for _ in range(5)],
        out_shape=[
            pltpu.VMEM((half, count * RANK), BF16),
            pltpu.VMEM((rows, MATS * cols), BF16),
            pltpu.VMEM((len(state), *state[0].shape), F32),
            pltpu.VMEM((half, width), BF16),
            pltpu.VMEM((width, RANK), BF16),
        ],
        scratch_shapes=[
            pltpu.VMEM((half, width), BF16),
            pltpu.VMEM((count, width, RANK), BF16),
            pltpu.VMEM((MATS, rows, cols), F32),
            pltpu.VMEM((half, count * RANK), F32),
            pltpu.SemaphoreType.DMA((len(IN_CUTS) - 1, 1 + count)),
            pltpu.SemaphoreType.DMA((MATS,)),
            pltpu.SemaphoreType.DMA((len(state),)),
            pltpu.SemaphoreType.DMA((2,)),
        ],
        compiler_params=params(),
        cost_estimate=cost(2 * half * RANK * width * count, 6 << 20),
        name="reduce_in",
    )(core, *in_hbm(source, *bases, *weights, grad, ob, *state))


def reduce_out_kernel(core, own, qc, fc, mixed, source, basis, out, sums):
    mine = half_of(core[0], out.shape[0])
    out[...] = jnp.dot(source[...], basis[...], preferred_element_type=F32).astype(BF16)
    for m, cotangent in enumerate((qc, fc)):
        sums[m] = contract_rows(own[:, m * RANK : (m + 1) * RANK], cotangent[mine, :])
    sums[2] = contract_rows(out[...], mixed[mine, :])


def reduce_out(core, own, cotangents, source, basis):
    half, width = source.shape
    cols = cotangents[0].shape[1]
    return pl.pallas_call(
        reduce_out_kernel,
        in_specs=[SMEM, *(VMEM for _ in range(3 + MATS))],
        out_specs=[VMEM, VMEM],
        out_shape=[pltpu.VMEM((half, RANK), BF16), pltpu.VMEM((MATS, RANK, cols), F32)],
        compiler_params=params(),
        cost_estimate=cost(2 * half * RANK * (width + 3 * cols), 6 << 20),
        name="reduce_out",
    )(core, *in_vmem(own, *cotangents, source, basis))


def contract_one(sums, other, cotangent, theirs, m, k):
    return sums[m] + contract_rows(other[:, k * RANK : (k + 1) * RANK], cotangent[theirs, :])


def contract_near_kernel(core, sums, other, qc, fc, out, held, sems):
    groups, rows = out.shape[0], out.shape[1] // MATS
    theirs = half_of(1 - core[0], other.shape[0])
    copies = []
    for m, cotangent in enumerate((qc, fc)):
        total = contract_one(sums, other, cotangent, theirs, m, m)
        held[m] = total.astype(BF16).reshape(groups, rows, total.shape[1])
        copies.append(
            pltpu.make_async_copy(held.at[m], out.at[:, m * rows : (m + 1) * rows, :], sems.at[m])
        )
        copies[m].start()
    for copy in copies:
        copy.wait()


def contract_near(core, sums, other, cotangents, groups):
    cols = sums.shape[2]
    rows = RANK // groups
    return pl.pallas_call(
        contract_near_kernel,
        in_specs=[SMEM, *(VMEM for _ in range(4))],
        out_specs=HBM,
        out_shape=pltpu.HBM((groups, MATS * rows, cols), BF16),
        scratch_shapes=[
            pltpu.VMEM((2, groups, rows, cols), BF16),
            pltpu.SemaphoreType.DMA((2,)),
        ],
        compiler_params=params(),
        cost_estimate=cost(4 * other.shape[0] * RANK * cols, 2 << 20),
        name="contract_near",
    )(core, *in_vmem(sums, other, *cotangents[:2]))


def contract_far_kernel(core, sums, other, mixed, _, out, held, sems):
    groups, rows = out.shape[0], out.shape[1] // MATS
    theirs = half_of(1 - core[0], other.shape[0])
    total = contract_one(sums, other, mixed, theirs, 2, 0)
    held[...] = total.astype(BF16).reshape(groups, rows, total.shape[1])
    copy = pltpu.make_async_copy(held, out.at[:, 2 * rows : 3 * rows, :], sems.at[0])
    copy.start()
    copy.wait()


def contract_far(core, sums, other, mixed, blocks):
    groups, rows, cols = blocks.shape
    return pl.pallas_call(
        contract_far_kernel,
        in_specs=[SMEM, *(VMEM for _ in range(3)), HBM],
        out_specs=HBM,
        out_shape=pltpu.HBM(blocks.shape, BF16),
        scratch_shapes=[
            pltpu.VMEM((groups, rows // MATS, cols), BF16),
            pltpu.SemaphoreType.DMA((1,)),
        ],
        input_output_aliases={4: 0},
        compiler_params=params(),
        cost_estimate=cost(2 * other.shape[0] * RANK * cols, 1 << 20),
        name="contract_far",
    )(core, *in_vmem(sums, other, mixed), *in_hbm(blocks))


def moment_kernel(arrived, held, *refs):
    state_new = refs[: 2 * MATS]
    directions, direction, held_new, sems, state_sems = refs[2 * MATS :]
    groups = arrived.shape[0]
    rows = arrived.shape[1] // MATS
    for m in range(MATS):
        at = slice(m * rows, (m + 1) * rows)
        value = arrived[0, at, :].astype(F32)
        for g in range(1, groups):
            value = value + arrived[g, at, :].astype(F32)
        first_new = 0.8 * held[m] + 0.2 * value
        second_new = 0.95 * held[MATS + m] + 0.05 * value * value
        held_new[m] = first_new
        held_new[MATS + m] = second_new
        direction[at, :] = (first_new / (jnp.sqrt(second_new) + 1e-08)).astype(BF16)
    sends = [
        pltpu.make_async_copy(direction, directions.at[g], sems.at[g]) for g in range(groups)
    ]
    sends += [
        pltpu.make_async_copy(held_new.at[n], ref, state_sems.at[n])
        for n, ref in enumerate(state_new)
    ]
    for send in sends:
        send.start()
    for send in sends:
        send.wait()


def moments(arrived, packed):
    groups, rows, cols = arrived.shape
    count = packed.shape[0]
    results = pl.pallas_call(
        moment_kernel,
        in_specs=[VMEM, VMEM],
        out_specs=[HBM for _ in range(count + 1)],
        out_shape=[
            *(pltpu.HBM(packed.shape[1:], F32) for _ in range(count)),
            pltpu.HBM(arrived.shape, BF16),
        ],
        scratch_shapes=[
            pltpu.VMEM((rows, cols), BF16),
            pltpu.VMEM(packed.shape, F32),
            pltpu.SemaphoreType.DMA((groups,)),
            pltpu.SemaphoreType.DMA((count,)),
        ],
        compiler_params=params(),
        cost_estimate=cost(1 << 22, 1 << 20),
        name="moments",
    )(*in_vmem(arrived, packed))
    return results[:count], results[count]


def collect_kernel(*refs):
    for k, block in enumerate(refs[: len(FAR)]):
        refs[len(FAR)][k] = block[...]


def collected(blocks):
    return pl.pallas_call(
        collect_kernel,
        in_specs=[VMEM for _ in blocks],
        out_specs=VMEM,
        out_shape=pltpu.HBM((len(blocks), *blocks[0].shape), BF16),
        compiler_params=params(),
        cost_estimate=cost(1 << 20, 2 << 20),
        name="collected",
    )(*in_vmem(*blocks))


def square_kernel(gathered, out):
    rows = gathered.shape[1] // MATS
    out[...] = jnp.zeros_like(out)
    for m in range(MATS):
        values = gathered[:, m * rows : (m + 1) * rows, :].astype(F32)
        total = jnp.sum(values * values)
        out[m : m + 1, :] = jnp.full((1, out.shape[1]), total, F32)


def squares(gathered):
    return pl.pallas_call(
        square_kernel,
        out_shape=jax.ShapeDtypeStruct((8, 128), F32),
        compiler_params=params(),
        cost_estimate=cost(1 << 22, 1 << 19),
        name="squares",
    )(gathered)


def step_kernel(gathered, qb, fb, ob, out, held, sems):
    rank_rows, cols = gathered.shape[1] // MATS, gathered.shape[2]
    copies = [
        pltpu.make_async_copy(b, held.at[m], sems.at[m]) for m, b in enumerate((qb, fb, ob))
    ]
    for copy in copies:
        copy.start()
    for m, copy in enumerate(copies):
        direction = gathered[:, m * rank_rows : (m + 1) * rank_rows, :].reshape(RANK, cols)
        copy.wait()

        def piece(i, carry):
            at = pl.ds(pl.multiple_of(i * 512, 512), 512)
            out[m, at, :] = jnp.dot(held[m, at, :], direction, preferred_element_type=F32)
            return carry

        lax.fori_loop(0, held.shape[1] // 512, piece, 0)


def steps(gathered, bases):
    width, cols = bases[0].shape[0], gathered.shape[2]
    return pl.pallas_call(
        step_kernel,
        in_specs=[VMEM, *(HBM for _ in bases)],
        out_specs=VMEM,
        out_shape=pltpu.VMEM((MATS, width, cols), F32),
        scratch_shapes=[
            pltpu.VMEM((MATS, width, RANK), BF16),
            pltpu.SemaphoreType.DMA((MATS,)),
        ],
        compiler_params=params(),
        cost_estimate=cost(MATS * 2 * width * RANK * cols, 9 << 20),
        name="steps",
    )(*in_vmem(gathered), *in_hbm(*bases))


def rows_at(me, near, j, rows):
    z = lax.rem(me[0] + 2 * SIDE - near[0] - 2 * lax.rem(j, 2), SIDE)
    y = lax.rem(me[1] + 2 * SIDE - near[1] - 2 * lax.div(j, 2), SIDE)
    return pl.ds(pl.multiple_of((z * SIDE + y) * rows, rows), rows)


def scale_of(totals, m):
    return lax.rsqrt(totals[m : m + 1, :1] * (1.0 / (RANK * WIDTH)) + 1e-06)


def updated(weight, j, m, factor, stepped, at):
    cols = stepped.shape[2]
    old = weight[j, :, m * cols : (m + 1) * cols].astype(F32)
    return (old - factor * stepped[m, at, :]).astype(BF16)


def apply_far_kernel(me, totals, stepped, four, *refs):
    updates, pieces, held, sems = refs[:MATS], refs[MATS], refs[MATS + 1], refs[MATS + 2]
    rows = held.shape[1]
    mine = pl.ds(pl.multiple_of((me[0] * SIDE + me[1]) * rows, rows), rows)
    stores = []
    for m in range(MATS):
        held[m] = stepped[m, mine, :] * scale_of(totals, m)
        stores.append(pltpu.make_async_copy(held.at[m], updates[m], sems.at[m]))
        stores[m].start()
    for m in range(MATS):
        factor = 0.05 * scale_of(totals, m)
        for j in range(len(FAR)):
            pieces[m, j] = updated(four, j, m, factor, stepped, rows_at(me, NEAR[0], j, rows))
    for store in stores:
        store.wait()


def apply_far(me, totals, stepped, four):
    cols = stepped.shape[2]
    count, rows = four.shape[:2]
    results = pl.pallas_call(
        apply_far_kernel,
        in_specs=[SMEM, VMEM, VMEM, VMEM],
        out_specs=[*(HBM for _ in range(MATS)), VMEM],
        out_shape=[
            *(pltpu.HBM((rows, cols), F32) for _ in range(MATS)),
            pltpu.VMEM((MATS, count, rows, cols), BF16),
        ],
        scratch_shapes=[
            pltpu.VMEM((MATS, rows, cols), F32),
            pltpu.SemaphoreType.DMA((MATS,)),
        ],
        compiler_params=params(),
        cost_estimate=cost(1 << 23, 3 << 20),
        name="apply_far",
    )(me, *in_vmem(totals, stepped, four))
    return results[:MATS], results[MATS]


def apply_near_kernel(me, totals, stepped, pieces, *refs):
    weights, copies, (held, sems) = refs[:MATS], refs[MATS : 2 * MATS], refs[2 * MATS :]
    rows = pieces.shape[2]
    stores = []
    for m in range(MATS):
        factor = 0.05 * scale_of(totals, m)

        def block(j, carry):
            held[m, rows_at(me, NEAR[0], j, rows), :] = pieces[m, j]
            for near, weight in zip(NEAR[1:], weights):
                at = rows_at(me, near, j, rows)
                held[m, at, :] = updated(weight, j, m, factor, stepped, at)
            return carry

        lax.fori_loop(0, len(FAR), block, 0)
        stores.append(pltpu.make_async_copy(held.at[m], copies[m], sems.at[m]))
        stores[m].start()
    for store in stores:
        store.wait()


def apply_near(me, totals, stepped, pieces, weights):
    width, cols = stepped.shape[1:]
    return pl.pallas_call(
        apply_near_kernel,
        in_specs=[SMEM, *(VMEM for _ in range(3 + len(weights)))],
        out_specs=[HBM for _ in range(MATS)],
        out_shape=[pltpu.HBM((width, cols), BF16) for _ in range(MATS)],
        scratch_shapes=[
            pltpu.VMEM((MATS, width, cols), BF16),
            pltpu.SemaphoreType.DMA((MATS,)),
        ],
        compiler_params=params(),
        cost_estimate=cost(1 << 24, 9 << 20),
        name="apply_near",
    )(me, *in_vmem(totals, stepped, pieces, *weights))


def moved_by(value, offset):
    pairs = []
    for z in range(SIDE):
        for y in range(SIDE):
            target = ((z + offset[0]) % SIDE) * SIDE + (y + offset[1]) % SIDE
            pairs.append((z * SIDE + y, target))
    return lax.ppermute(value, FS, pairs)


def gathered_by(value, offsets):
    moved = []
    for offset in offsets[1:]:
        moved.append(moved_by(value, offset))
    return moved


def summed_over_tp(value):
    value = value + lax.ppermute(value, "tp_1", [(0, 1), (1, 0)])
    arrived = [
        lax.ppermute(value, "tp_0", [(i, (i + far) % SIDE) for i in range(SIDE)])
        for far in (1, 2, 3)
    ]
    return value + (arrived[0] + arrived[2]) + arrived[1]


def body(
    saved_input,
    query_cotangent,
    forget_cotangent,
    mixed_output,
    out_cotangent,
    query_basis,
    forget_basis,
    out_basis,
    query_weight,
    forget_weight,
    out_weight,
    *state,
):
    groups = lax.axis_size(FS)
    bases = (query_basis, forget_basis, out_basis)
    cotangents = (query_cotangent, forget_cotangent, mixed_output)
    core = lax.axis_index("tp_1").astype(jnp.int32).reshape(1)
    me = jnp.stack([lax.axis_index("fs_0"), lax.axis_index("fs_1")]).astype(jnp.int32)

    own, weights, packed, grad_half, ob_held = reduce_in(
        core,
        saved_input,
        bases[:2],
        (query_weight, forget_weight, out_weight),
        out_cotangent,
        out_basis,
        state,
    )
    other = lax.ppermute(own, "tp_1", [(0, 1), (1, 0)])
    own_out, sums = reduce_out(core, own, cotangents, grad_half, ob_held)
    other_out = lax.ppermute(own_out, "tp_1", [(0, 1), (1, 0)])
    blocks = contract_near(core, sums, other, cotangents, groups)
    blocks = contract_far(core, sums, other_out, mixed_output, blocks)
    four = collected((weights, *gathered_by(weights, FAR)))
    near_weights = gathered_by(four, NEAR)

    arrived = lax.all_to_all(blocks, FS, 0, 0, tiled=True)
    state_new, directions = moments(arrived, packed)
    gathered = lax.all_to_all(directions, FS, 0, 0, tiled=True)
    totals = summed_over_tp(squares(gathered))
    stepped = steps(gathered, bases)
    updates, pieces = apply_far(me, totals, stepped, four)
    copies = apply_near(me, totals, stepped, pieces, near_weights)
    return (*updates, *state_new, *copies)


def solution(mesh):
    split = Mesh(mesh.devices.reshape(4, 4, 4, 2), ("fs_0", "fs_1", "tp_0", "tp_1"))
    in_specs = (
        P(FS, None),
        P(FS, TP),
        P(FS, TP),
        P(FS, TP),
        P(FS, None),
        P(),
        P(),
        P(),
        *(P(FS, TP) for _ in range(9)),
    )
    out_specs = (*(P(FS, TP) for _ in range(9)), *(P(None, TP) for _ in range(3)))
    return jax.shard_map(body, mesh=split, in_specs=in_specs, out_specs=out_specs, check_vma=False)
```

```python
import jax
import jax.numpy as jnp
from jax import lax
from jax.experimental import pallas as pl
from jax.experimental.pallas import tpu as pltpu
from jax.sharding import Mesh
from jax.sharding import PartitionSpec as P

WIDTH = 2048
RANK = 256
FS = ("fs_0", "fs_1")
TP = ("tp_0", "tp_1")
MATS = 3
IN_CUTS = (0, 1024, 2048)
SIDE = 4
GRANT = 24 * 1024 * 1024

F32 = jnp.float32
BF16 = jnp.bfloat16

FAR = ((0, 0), (2, 0), (0, 2), (2, 2))
NEAR = ((0, 0), (3, 0), (0, 3), (1, 1))


SMEM = pl.BlockSpec(memory_space=pltpu.SMEM)
VMEM = pl.BlockSpec(memory_space=pltpu.VMEM)
HBM = pl.BlockSpec(memory_space=pltpu.HBM)


def cost(flops, moved):
    return pl.CostEstimate(flops=flops, bytes_accessed=moved, transcendentals=0)


def params():
    return pltpu.CompilerParams(vmem_limit_bytes=GRANT)


def in_hbm(*arrays):
    return [pltpu.with_memory_space_constraint(a, pltpu.HBM) for a in arrays]


def in_vmem(*arrays):
    return [pltpu.with_memory_space_constraint(a, pltpu.VMEM) for a in arrays]


def contract_rows(left, right):
    return lax.dot_general(
        left, right, (((0,), (0,)), ((), ())), preferred_element_type=F32
    )


def half_of(which, half):
    return pl.ds(pl.multiple_of(which * half, half), half)


def reduce_in_kernel(core, source, qb, fb, qw, fw, ow, grad, ob, qc, fc, mixed, *refs):
    state, refs = refs[: 2 * MATS], refs[2 * MATS :]
    out, rounded, packed, grad_half, ob_held, cots = refs[:6]
    rows_in, basis_in, weights_in, sums, sems, weight_sems, state_sems, next_sems = refs[6:]
    bases, weights = (qb, fb), (qw, fw, ow)
    mine = half_of(core[0], out.shape[0])
    copies = []
    for c, (low, high) in enumerate(zip(IN_CUTS, IN_CUTS[1:])):
        at = slice(low, high)
        pieces = [(source.at[mine, at], rows_in.at[:, at])]
        pieces += [(b.at[at, :], basis_in.at[m, at, :]) for m, b in enumerate(bases)]
        copies.append(
            [pltpu.make_async_copy(a, b, sems.at[c, p]) for p, (a, b) in enumerate(pieces)]
        )
    weight_copies = [
        pltpu.make_async_copy(w, weights_in.at[m], weight_sems.at[m])
        for m, w in enumerate(weights)
    ]
    state_copies = [
        pltpu.make_async_copy(a, packed.at[n], state_sems.at[n]) for n, a in enumerate(state)
    ]
    next_copies = [
        pltpu.make_async_copy(grad.at[mine, :], grad_half, next_sems.at[0]),
        pltpu.make_async_copy(ob, ob_held, next_sems.at[1]),
        *(
            pltpu.make_async_copy(a.at[mine, :], cots.at[m], next_sems.at[2 + m])
            for m, a in enumerate((qc, fc, mixed))
        ),
    ]
    for copy in (*copies[0], *weight_copies, *copies[1]):
        copy.start()
    for c, (low, high) in enumerate(zip(IN_CUTS, IN_CUTS[1:])):
        at = slice(low, high)
        for copy in copies[c]:
            copy.wait()
        if c == 0:
            for copy in (*next_copies, *state_copies):
                copy.start()
        for m in range(len(bases)):
            to = slice(m * RANK, (m + 1) * RANK)
            part = jnp.dot(rows_in[:, at], basis_in[m, at, :], preferred_element_type=F32)
            if c == 0:
                sums[:, to] = part
            else:
                out[:, to] = (sums[:, to] + part).astype(BF16)
        if c == 0:
            cols = weights_in.shape[2]
            for m, copy in enumerate(weight_copies):
                copy.wait()
                rounded[:, m * cols : (m + 1) * cols] = weights_in[m].astype(BF16)
    for copy in (*state_copies, *next_copies):
        copy.wait()


def reduce_in(core, source, bases, weights, grad, ob, cotangents, state):
    tokens, width = source.shape
    half, count = tokens // 2, len(bases)
    rows, cols = weights[0].shape
    return pl.pallas_call(
        reduce_in_kernel,
        in_specs=[SMEM, *(HBM for _ in range(3 + count + 2 * MATS + len(state)))],
        out_specs=[VMEM for _ in range(6)],
        out_shape=[
            pltpu.VMEM((half, count * RANK), BF16),
            pltpu.VMEM((rows, MATS * cols), BF16),
            pltpu.VMEM((len(state), *state[0].shape), F32),
            pltpu.VMEM((half, width), BF16),
            pltpu.VMEM((width, RANK), BF16),
            pltpu.VMEM((MATS, half, cols), BF16),
        ],
        scratch_shapes=[
            pltpu.VMEM((half, width), BF16),
            pltpu.VMEM((count, width, RANK), BF16),
            pltpu.VMEM((MATS, rows, cols), F32),
            pltpu.VMEM((half, count * RANK), F32),
            pltpu.SemaphoreType.DMA((len(IN_CUTS) - 1, 1 + count)),
            pltpu.SemaphoreType.DMA((MATS,)),
            pltpu.SemaphoreType.DMA((len(state),)),
            pltpu.SemaphoreType.DMA((2 + MATS,)),
        ],
        compiler_params=params(),
        cost_estimate=cost(2 * half * RANK * width * count, 14 << 20),
        name="reduce_in",
    )(core, *in_hbm(source, *bases, *weights, grad, ob, *cotangents, *state))


def reduce_out_kernel(core, own, cots, source, basis, qc, fc, mixed, out, sums, rest, sems):
    theirs = half_of(1 - core[0], out.shape[0])
    copies = [
        pltpu.make_async_copy(a.at[theirs, :], rest.at[m], sems.at[m])
        for m, a in enumerate((qc, fc, mixed))
    ]
    for copy in copies:
        copy.start()
    out[...] = jnp.dot(source[...], basis[...], preferred_element_type=F32).astype(BF16)
    for m in range(2):
        sums[m] = contract_rows(own[:, m * RANK : (m + 1) * RANK], cots[m])
    sums[2] = contract_rows(out[...], cots[2])
    for copy in copies:
        copy.wait()


def reduce_out(core, own, cots, source, basis, cotangents):
    half, width = source.shape
    cols = cots.shape[2]
    return pl.pallas_call(
        reduce_out_kernel,
        in_specs=[SMEM, *(VMEM for _ in range(4)), *(HBM for _ in cotangents)],
        out_specs=[VMEM for _ in range(3)],
        out_shape=[
            pltpu.VMEM((half, RANK), BF16),
            pltpu.VMEM((MATS, RANK, cols), F32),
            pltpu.VMEM(cots.shape, BF16),
        ],
        scratch_shapes=[pltpu.SemaphoreType.DMA((MATS,))],
        compiler_params=params(),
        cost_estimate=cost(2 * half * RANK * (width + 3 * cols), 6 << 20),
        name="reduce_out",
    )(core, *in_vmem(own, cots, source, basis), *in_hbm(*cotangents))


def contract_near_kernel(sums, other, cots, out, held, sems):
    groups, rows = out.shape[0], out.shape[1] // MATS
    copies = []
    for m in range(2):
        total = sums[m] + contract_rows(other[:, m * RANK : (m + 1) * RANK], cots[m])
        held[m] = total.astype(BF16).reshape(groups, rows, total.shape[1])
        copies.append(
            pltpu.make_async_copy(held.at[m], out.at[:, m * rows : (m + 1) * rows, :], sems.at[m])
        )
        copies[m].start()
    for copy in copies:
        copy.wait()


def contract_near(sums, other, cots, groups):
    cols = sums.shape[2]
    rows = RANK // groups
    return pl.pallas_call(
        contract_near_kernel,
        in_specs=[VMEM for _ in range(3)],
        out_specs=HBM,
        out_shape=pltpu.HBM((groups, MATS * rows, cols), BF16),
        scratch_shapes=[
            pltpu.VMEM((2, groups, rows, cols), BF16),
            pltpu.SemaphoreType.DMA((2,)),
        ],
        compiler_params=params(),
        cost_estimate=cost(4 * other.shape[0] * RANK * cols, 2 << 20),
        name="contract_near",
    )(*in_vmem(sums, other, cots))


def contract_far_kernel(sums, other, cots, _, out, held, sems):
    groups, rows = out.shape[0], out.shape[1] // MATS
    total = sums[2] + contract_rows(other[...], cots[2])
    held[...] = total.astype(BF16).reshape(groups, rows, total.shape[1])
    copy = pltpu.make_async_copy(held, out.at[:, 2 * rows : 3 * rows, :], sems.at[0])
    copy.start()
    copy.wait()


def contract_far(sums, other, cots, blocks):
    groups, rows, cols = blocks.shape
    return pl.pallas_call(
        contract_far_kernel,
        in_specs=[*(VMEM for _ in range(3)), HBM],
        out_specs=HBM,
        out_shape=pltpu.HBM(blocks.shape, BF16),
        scratch_shapes=[
            pltpu.VMEM((groups, rows // MATS, cols), BF16),
            pltpu.SemaphoreType.DMA((1,)),
        ],
        input_output_aliases={3: 0},
        compiler_params=params(),
        cost_estimate=cost(2 * other.shape[0] * RANK * cols, 1 << 20),
        name="contract_far",
    )(*in_vmem(sums, other, cots), *in_hbm(blocks))


def moment_kernel(arrived, held, *refs):
    state_new = refs[: 2 * MATS]
    directions, direction, held_new, sems, state_sems = refs[2 * MATS :]
    groups = arrived.shape[0]
    rows = arrived.shape[1] // MATS
    for m in range(MATS):
        at = slice(m * rows, (m + 1) * rows)
        value = arrived[0, at, :].astype(F32)
        for g in range(1, groups):
            value = value + arrived[g, at, :].astype(F32)
        first_new = 0.8 * held[m] + 0.2 * value
        second_new = 0.95 * held[MATS + m] + 0.05 * value * value
        held_new[m] = first_new
        held_new[MATS + m] = second_new
        direction[at, :] = (first_new / (jnp.sqrt(second_new) + 1e-08)).astype(BF16)
    sends = [
        pltpu.make_async_copy(direction, directions.at[g], sems.at[g]) for g in range(groups)
    ]
    sends += [
        pltpu.make_async_copy(held_new.at[n], ref, state_sems.at[n])
        for n, ref in enumerate(state_new)
    ]
    for send in sends:
        send.start()
    for send in sends:
        send.wait()


def moments(arrived, packed):
    groups, rows, cols = arrived.shape
    count = packed.shape[0]
    results = pl.pallas_call(
        moment_kernel,
        in_specs=[VMEM, VMEM],
        out_specs=[HBM for _ in range(count + 1)],
        out_shape=[
            *(pltpu.HBM(packed.shape[1:], F32) for _ in range(count)),
            pltpu.HBM(arrived.shape, BF16),
        ],
        scratch_shapes=[
            pltpu.VMEM((rows, cols), BF16),
            pltpu.VMEM(packed.shape, F32),
            pltpu.SemaphoreType.DMA((groups,)),
            pltpu.SemaphoreType.DMA((count,)),
        ],
        compiler_params=params(),
        cost_estimate=cost(1 << 22, 1 << 20),
        name="moments",
    )(*in_vmem(arrived, packed))
    return results[:count], results[count]


def collect_kernel(*refs):
    for k, block in enumerate(refs[: len(FAR)]):
        refs[len(FAR)][k] = block[...]


def collected(blocks):
    return pl.pallas_call(
        collect_kernel,
        in_specs=[VMEM for _ in blocks],
        out_specs=VMEM,
        out_shape=pltpu.HBM((len(blocks), *blocks[0].shape), BF16),
        compiler_params=params(),
        cost_estimate=cost(1 << 20, 2 << 20),
        name="collected",
    )(*in_vmem(*blocks))


def square_kernel(gathered, out):
    rows = gathered.shape[1] // MATS
    out[...] = jnp.zeros_like(out)
    for m in range(MATS):
        values = gathered[:, m * rows : (m + 1) * rows, :].astype(F32)
        total = jnp.sum(values * values)
        out[m : m + 1, :] = jnp.full((1, out.shape[1]), total, F32)


def squares(gathered):
    return pl.pallas_call(
        square_kernel,
        out_shape=jax.ShapeDtypeStruct((8, 128), F32),
        compiler_params=params(),
        cost_estimate=cost(1 << 22, 1 << 19),
        name="squares",
    )(gathered)


def step_kernel(gathered, qb, fb, ob, out, held, sems):
    rank_rows, cols = gathered.shape[1] // MATS, gathered.shape[2]
    copies = [
        pltpu.make_async_copy(b, held.at[m], sems.at[m]) for m, b in enumerate((qb, fb, ob))
    ]
    for copy in copies:
        copy.start()
    for m, copy in enumerate(copies):
        direction = gathered[:, m * rank_rows : (m + 1) * rank_rows, :].reshape(RANK, cols)
        copy.wait()

        def piece(i, carry):
            at = pl.ds(pl.multiple_of(i * 512, 512), 512)
            out[m, at, :] = jnp.dot(held[m, at, :], direction, preferred_element_type=F32)
            return carry

        lax.fori_loop(0, held.shape[1] // 512, piece, 0)


def steps(gathered, bases):
    width, cols = bases[0].shape[0], gathered.shape[2]
    return pl.pallas_call(
        step_kernel,
        in_specs=[VMEM, *(HBM for _ in bases)],
        out_specs=VMEM,
        out_shape=pltpu.VMEM((MATS, width, cols), F32),
        scratch_shapes=[
            pltpu.VMEM((MATS, width, RANK), BF16),
            pltpu.SemaphoreType.DMA((MATS,)),
        ],
        compiler_params=params(),
        cost_estimate=cost(MATS * 2 * width * RANK * cols, 9 << 20),
        name="steps",
    )(*in_vmem(gathered), *in_hbm(*bases))


def rows_at(me, near, j, rows):
    z = lax.rem(me[0] + 2 * SIDE - near[0] - 2 * lax.rem(j, 2), SIDE)
    y = lax.rem(me[1] + 2 * SIDE - near[1] - 2 * lax.div(j, 2), SIDE)
    return pl.ds(pl.multiple_of((z * SIDE + y) * rows, rows), rows)


def scale_of(totals, m):
    return lax.rsqrt(totals[m : m + 1, :1] * (1.0 / (RANK * WIDTH)) + 1e-06)


def updated(weight, j, m, change, at):
    cols = change.shape[2]
    old = weight[j, :, m * cols : (m + 1) * cols].astype(F32)
    return (old - change[m, at, :]).astype(BF16)


def apply_far_kernel(me, totals, stepped, four, *refs):
    updates, (pieces, change, held, sems) = refs[:MATS], refs[MATS:]
    rows = held.shape[1]
    mine = pl.ds(pl.multiple_of((me[0] * SIDE + me[1]) * rows, rows), rows)
    stores = []
    for m in range(MATS):
        held[m] = stepped[m, mine, :] * scale_of(totals, m)
        stores.append(pltpu.make_async_copy(held.at[m], updates[m], sems.at[m]))
        stores[m].start()
    for m in range(MATS):
        change[m] = (0.05 * scale_of(totals, m)) * stepped[m]
        for j in range(len(FAR)):
            pieces[m, j] = updated(four, j, m, change, rows_at(me, NEAR[0], j, rows))
    for store in stores:
        store.wait()


def apply_far(me, totals, stepped, four):
    cols = stepped.shape[2]
    count, rows = four.shape[:2]
    results = pl.pallas_call(
        apply_far_kernel,
        in_specs=[SMEM, VMEM, VMEM, VMEM],
        out_specs=[*(HBM for _ in range(MATS)), VMEM, VMEM],
        out_shape=[
            *(pltpu.HBM((rows, cols), F32) for _ in range(MATS)),
            pltpu.VMEM((MATS, count, rows, cols), BF16),
            pltpu.VMEM(stepped.shape, F32),
        ],
        scratch_shapes=[
            pltpu.VMEM((MATS, rows, cols), F32),
            pltpu.SemaphoreType.DMA((MATS,)),
        ],
        compiler_params=params(),
        cost_estimate=cost(1 << 23, 3 << 20),
        name="apply_far",
    )(me, *in_vmem(totals, stepped, four))
    return results[:MATS], results[MATS], results[MATS + 1]


def apply_near_kernel(me, change, pieces, *refs):
    weights, copies, (held, sems) = refs[:MATS], refs[MATS : 2 * MATS], refs[2 * MATS :]
    rows = pieces.shape[2]
    stores = []
    for m in range(MATS):

        def block(j, carry):
            held[m, rows_at(me, NEAR[0], j, rows), :] = pieces[m, j]
            for near, weight in zip(NEAR[1:], weights):
                at = rows_at(me, near, j, rows)
                held[m, at, :] = updated(weight, j, m, change, at)
            return carry

        lax.fori_loop(0, len(FAR), block, 0)
        stores.append(pltpu.make_async_copy(held.at[m], copies[m], sems.at[m]))
        stores[m].start()
    for store in stores:
        store.wait()


def apply_near(me, change, pieces, weights):
    width, cols = change.shape[1:]
    return pl.pallas_call(
        apply_near_kernel,
        in_specs=[SMEM, *(VMEM for _ in range(2 + len(weights)))],
        out_specs=[HBM for _ in range(MATS)],
        out_shape=[pltpu.HBM((width, cols), BF16) for _ in range(MATS)],
        scratch_shapes=[
            pltpu.VMEM((MATS, width, cols), BF16),
            pltpu.SemaphoreType.DMA((MATS,)),
        ],
        compiler_params=params(),
        cost_estimate=cost(1 << 24, 9 << 20),
        name="apply_near",
    )(me, *in_vmem(change, pieces, *weights))


def moved_by(value, offset):
    pairs = []
    for z in range(SIDE):
        for y in range(SIDE):
            target = ((z + offset[0]) % SIDE) * SIDE + (y + offset[1]) % SIDE
            pairs.append((z * SIDE + y, target))
    return lax.ppermute(value, FS, pairs)


def gathered_by(value, offsets):
    moved = []
    for offset in offsets[1:]:
        moved.append(moved_by(value, offset))
    return moved


def summed_over_tp(value):
    value = value + lax.ppermute(value, "tp_1", [(0, 1), (1, 0)])
    arrived = [
        lax.ppermute(value, "tp_0", [(i, (i + far) % SIDE) for i in range(SIDE)])
        for far in (1, 2, 3)
    ]
    return value + (arrived[0] + arrived[2]) + arrived[1]


def body(
    saved_input,
    query_cotangent,
    forget_cotangent,
    mixed_output,
    out_cotangent,
    query_basis,
    forget_basis,
    out_basis,
    query_weight,
    forget_weight,
    out_weight,
    *state,
):
    groups = lax.axis_size(FS)
    bases = (query_basis, forget_basis, out_basis)
    cotangents = (query_cotangent, forget_cotangent, mixed_output)
    core = lax.axis_index("tp_1").astype(jnp.int32).reshape(1)
    me = jnp.stack([lax.axis_index("fs_0"), lax.axis_index("fs_1")]).astype(jnp.int32)

    own, weights, packed, grad_half, ob_held, cots = reduce_in(
        core,
        saved_input,
        bases[:2],
        (query_weight, forget_weight, out_weight),
        out_cotangent,
        out_basis,
        cotangents,
        state,
    )
    other = lax.ppermute(own, "tp_1", [(0, 1), (1, 0)])
    own_out, sums, rest = reduce_out(core, own, cots, grad_half, ob_held, cotangents)
    other_out = lax.ppermute(own_out, "tp_1", [(0, 1), (1, 0)])
    blocks = contract_near(sums, other, rest, groups)
    blocks = contract_far(sums, other_out, rest, blocks)
    four = collected((weights, *gathered_by(weights, FAR)))
    near_weights = gathered_by(four, NEAR)

    arrived = lax.all_to_all(blocks, FS, 0, 0, tiled=True)
    state_new, directions = moments(arrived, packed)
    gathered = lax.all_to_all(directions, FS, 0, 0, tiled=True)
    totals = summed_over_tp(squares(gathered))
    stepped = steps(gathered, bases)
    updates, pieces, change = apply_far(me, totals, stepped, four)
    copies = apply_near(me, change, pieces, near_weights)
    return (*updates, *state_new, *copies)


def solution(mesh):
    split = Mesh(mesh.devices.reshape(4, 4, 4, 2), ("fs_0", "fs_1", "tp_0", "tp_1"))
    in_specs = (
        P(FS, None),
        P(FS, TP),
        P(FS, TP),
        P(FS, TP),
        P(FS, None),
        P(),
        P(),
        P(),
        *(P(FS, TP) for _ in range(9)),
    )
    out_specs = (*(P(FS, TP) for _ in range(9)), *(P(None, TP) for _ in range(3)))
    return jax.shard_map(body, mesh=split, in_specs=in_specs, out_specs=out_specs, check_vma=False)
```
